256 devices in a mesh: sp: 16 (over y, x), tp: 16 (over z, core).
Axes of the slice: x: 4, y: 4, z: 8, core: 2. Of those that a mesh axis runs over, the one named last changes fastest.
Arguments:
- conv_value: bfloat16 [1024, 16384], P('tp', 'sp'), may hold values from -6 to 6
- conv_gate: bfloat16 [1024, 16384], P('tp', 'sp'), may hold values from -6 to 6
- conv_taps: float32 [1024, 31], P('tp'), may hold values from -2.2 to 2.2
- norm_gain: float32 [1024], replicated, may hold values from 0.1 to 1.9
- norm_bias: float32 [1024], replicated, may hold values from -3 to 3
- out_weight: bfloat16 [1024, 2048], replicated, may hold values from -0.1875 to 0.1875
- stream: bfloat16 [16384, 2048], P(('sp', 'tp')), may hold values from -6 to 6
- routes: int32 [16384, 2], P(('sp', 'tp')), may hold values from 0 to 15, all different within a row; in each aligned block of 64 rows (0 to 63, 64 to 127, ...) at most 8 rows name the same one
- route_weights: float32 [16384, 2], P(('sp', 'tp')), may hold values from 0.2 to 1
- expert_gain: float32 [2048], replicated, may hold values from 0.1 to 1.9
- expert_gate: bfloat16 [16, 2048, 7168], P('sp', None, 'tp'), may hold values from -0.125 to 0.125
- expert_up: bfloat16 [16, 2048, 7168], P('sp', None, 'tp'), may hold values from -0.125 to 0.125
- expert_down: bfloat16 [16, 7168, 2048], P('sp', 'tp'), may hold values from -0.0625 to 0.0625
Outputs:
- mixed: bfloat16 [16384, 2048], P(('sp', 'tp'))
The draws below stay inside these ranges and needn't reach their ends.
Inputs may be any that keep to these rules, and one draw needn't show every extreme that they name: `routes`: within each device's 64 rows every expert is named exactly 8 times; a row names distinct experts.
All inputs are finite; a program needn't handle non-finite values.
Results may differ from the reference program's by a relative error of at most 0.014.
Values may be sent and summed in bfloat16 or wider, within the bound.
No kernel may reach another device: no remote copies, remote signals or barrier semaphores. Data moves between devices by JAX's collectives and lax.ppermute only.
A program may use at most 64 MiB of HBM per device.

```python
import math
import jax
import jax.numpy as jnp
import numpy as np
from jax import lax

D = 2048
CONV_CH = 1024
KERNEL = 31
FF_E = 7168
TOP = 2
TOK_DEV = 64
EXPERTS = 16
CAP = 8
TOKENS = 16384
N_TP = 16


def draw_conv_taps(key, part):
    base = jnp.clip(jax.random.normal(key, (CONV_CH, KERNEL), jnp.float32), -4.0, 4.0)
    scales = jnp.exp(jnp.linspace(math.log(0.5), math.log(3.0), CONV_CH))
    return (base * scales[:, None] * KERNEL ** (-0.5)).astype(jnp.float32)


def block_levels(stream_key, shape, pieces, low, high):
    factor_of, own = 1.0, jax.random.fold_in(stream_key, 6)
    for axis_at, shards_of in pieces:
        steps = jnp.exp(jax.random.uniform(jax.random.fold_in(own, axis_at), (shards_of,), jnp.float32, low / len(pieces), high / len(pieces)))
        factor_of = factor_of * jnp.repeat(steps, shape[axis_at] // shards_of).reshape([-1 if axis == axis_at else 1 for axis in range(len(shape))])
    return factor_of


def routed_block(stream_key, own, number, rows, count, top, bound, lean):
    ranking = jax.random.permutation(stream_key, count)
    heavy_load, usual = shares(count, rows * top, bound, lean, True), shares(count, rows * top, bound, lean, False)
    places = jnp.arange(count)

    def named(tallies, rotation):
        used = int((tallies > 0).sum())
        fixed = max(1, used // 4)
        moved = fixed + (places - fixed + rotation * (used - fixed)) % max(1, count - fixed)
        return jnp.zeros((count,), jnp.int32).at[ranking[jnp.where(places < fixed, places, moved)]].set(jnp.asarray(tallies, jnp.int32))

    tallies = jnp.where(number % 4 == 0, named(heavy_load, number // 4), named(usual, number - number // 4 - 1))
    mixed = jax.random.permutation(jax.random.fold_in(own, 3), count)
    donor, taker = mixed[0:count // 2 * 2:2], mixed[1:count // 2 * 2:2]
    margin = jnp.minimum(tallies[donor] - 1, bound - tallies[taker]) // 2
    margin = jnp.where((donor == ranking[0]) | (taker == ranking[0]) | (tallies[taker] == 0), 0, jnp.maximum(margin, 0))
    moved = jax.random.randint(jax.random.fold_in(own, 4), (count // 2,), 0, 1 << 20) % (margin + 1)
    tallies = tallies.at[donor].add(-moved).at[taker].add(moved)
    members = jnp.searchsorted(jnp.cumsum(tallies), jnp.arange(rows * top), side="right").astype(jnp.int32)
    listing = members.reshape(top, rows).T
    listing = listing[jax.random.permutation(jax.random.fold_in(own, 1), rows)]
    rotation = jax.random.randint(jax.random.fold_in(own, 2), (rows, 1), 0, top)
    return jnp.take_along_axis(listing, (jnp.arange(top)[None, :] + rotation) % top, axis=1)


def shares(number_of, total, bound, lean, full):
    loads = [(1 << 20) // math.isqrt(grade ** lean) + 1 for grade in range(1, number_of + 1)]
    largest = bound if full else min(bound, max(-(-total // number_of), total * loads[0] // sum(loads)))
    least = 1 if total - largest >= number_of - 1 else 0
    given, rest = [largest] + [least] * (number_of - 1), total - largest - least * (number_of - 1)
    while rest > 0:
        candidates = [i for i in range(1, number_of) if given[i] < largest] or [i for i in range(1, number_of) if given[i] < bound]
        pool, left = sum([loads[i] for i in candidates]), rest
        for i in candidates:
            extra = min(bound - given[i], max(1, left * loads[i] // pool), rest)
            given[i] = given[i] + extra
            rest = rest - extra
    return np.array(given)


def normal_values(own_key, shape, scale, limit, pieces=(), kind=jnp.bfloat16):
    drawn = scale * jax.random.normal(own_key, shape, jnp.float32)
    if pieces:
        drawn = drawn * block_levels(own_key, shape, pieces, -0.22, 0.18)
    return jnp.clip(drawn, -limit, limit).astype(kind)


def setup_inputs(seed: int = 0) -> dict:
    key_of = jax.random.split(jax.random.key(seed), 14)
    conv_value = normal_values(key_of[0], (CONV_CH, TOKENS), 1.0, 6.0, ((0, 16), (1, 16)))
    conv_gate = normal_values(key_of[1], (CONV_CH, TOKENS), 1.5, 6.0, ((0, 16), (1, 16)))
    conv_taps = draw_conv_taps(jax.random.fold_in(key_of[13], 71), 0)
    norm_gain = jnp.clip(1.0 + 0.18 * jax.random.normal(key_of[3], (CONV_CH,), jnp.float32), 0.1, 1.9)
    norm_bias = normal_values(key_of[4], (CONV_CH,), 0.5, 3.0, (), jnp.float32)
    out_weight = normal_values(key_of[5], (CONV_CH, D), CONV_CH ** -0.5, 0.1875)
    stream = normal_values(key_of[6], (TOKENS, D), 1.0, 6.0, ((0, 256),))
    routes_keys = jax.random.split(jax.random.fold_in(key_of[7], 1), TOKENS // TOK_DEV)
    routes_turns = jax.random.permutation(jax.random.fold_in(key_of[7], 3), TOKENS // TOK_DEV)
    routes = jax.vmap(lambda own, number: routed_block(jax.random.fold_in(key_of[7], 2), own, number, TOK_DEV, EXPERTS, TOP, CAP, 0))(routes_keys, routes_turns).reshape((TOKENS, TOP))
    route_weights = jnp.clip(0.2 + 0.8 * jax.random.uniform(key_of[8], (TOKENS, TOP), jnp.float32) ** block_levels(key_of[8], (TOKENS, TOP), ((0, 256),), -0.2, 0.2), 0.2, 1.0)
    expert_gain = jnp.clip(1.0 + 0.18 * jax.random.normal(key_of[9], (D,), jnp.float32), 0.1, 1.9)
    expert_gate = normal_values(key_of[10], (EXPERTS, D, FF_E), D ** -0.5, 0.125, ((0, 16), (2, 16)))
    expert_up = normal_values(key_of[11], (EXPERTS, D, FF_E), D ** -0.5, 0.125, ((0, 16), (2, 16)))
    expert_down = normal_values(key_of[12], (EXPERTS, FF_E, D), FF_E ** -0.5, 0.0625, ((0, 16), (1, 16)))
    return dict(conv_value=conv_value, conv_gate=conv_gate, conv_taps=conv_taps, norm_gain=norm_gain, norm_bias=norm_bias, out_weight=out_weight, stream=stream, routes=routes, route_weights=route_weights, expert_gain=expert_gain, expert_gate=expert_gate, expert_up=expert_up, expert_down=expert_down)


epsilon = 1e-06

def reference(conv_value, conv_gate, conv_taps, norm_gain, norm_bias, out_weight, stream, routes, route_weights, expert_gain, expert_gate, expert_up, expert_down):
    f32 = jnp.float32
    gated_input = (conv_value.astype(f32) * jax.nn.sigmoid(conv_gate.astype(f32))).astype(jnp.bfloat16)
    padded = jnp.pad(gated_input.astype(f32), ((0, 0), (KERNEL - 1, 0)))
    conv_sum = jnp.zeros((CONV_CH, TOKENS), f32)
    for offset in range(KERNEL):
        conv_sum = conv_sum + conv_taps[:, offset:offset + 1] * padded[:, offset:offset + TOKENS]
    conv_float = lax.optimization_barrier(conv_sum.astype(jnp.bfloat16)).astype(f32)
    center = lax.optimization_barrier(jnp.mean(conv_float, axis=0, keepdims=True))
    spread = lax.optimization_barrier(jnp.mean((conv_float - center) ** 2, axis=0, keepdims=True))
    scaled = (conv_float - center) * lax.rsqrt(spread + epsilon) * norm_gain[:, None] + norm_bias[:, None]
    activated = jax.nn.silu(scaled).astype(jnp.bfloat16)
    projected = lax.dot_general(activated, out_weight, (((0,), (0,)), ((), ())), preferred_element_type=f32)
    residual = (stream.astype(f32) + projected).astype(jnp.bfloat16)
    res_float = residual.astype(f32)
    normed = (res_float * lax.rsqrt(lax.optimization_barrier(jnp.mean(res_float * res_float, axis=1, keepdims=True)) + epsilon) * expert_gain).astype(jnp.bfloat16)
    blocks = TOKENS // TOK_DEV
    flat_ids = routes.reshape(blocks, TOK_DEV * TOP)
    onehot = (flat_ids[:, :, None] == jnp.arange(EXPERTS, dtype=jnp.int32)[None, None, :]).astype(jnp.int32)
    before = jnp.cumsum(onehot, axis=1) - onehot
    rank = lax.optimization_barrier(jnp.sum(before * onehot, axis=2))
    row_slot = jnp.arange(blocks, dtype=jnp.int32)[:, None] * CAP + rank
    token_of = (jnp.arange(blocks, dtype=jnp.int32)[:, None] * TOK_DEV + jnp.arange(TOK_DEV * TOP, dtype=jnp.int32)[None, :] // TOP).astype(jnp.int32)
    table = jnp.full((EXPERTS, blocks * CAP), TOKENS, jnp.int32).at[flat_ids, row_slot].set(token_of)
    weight_table = jnp.zeros((EXPERTS, blocks * CAP), f32).at[flat_ids, row_slot].set(route_weights.reshape(blocks, TOK_DEV * TOP))
    padded_rows = jnp.concatenate([normed, jnp.zeros((1, D), jnp.bfloat16)], axis=0)
    width_block = FF_E // N_TP

    def per_expert(total, inputs):
        index, weights, gate_w, up_w, down_w = inputs
        rows = padded_rows[index]
        gate_val = jnp.dot(rows, gate_w, preferred_element_type=f32)
        up_val = jnp.dot(rows, up_w, preferred_element_type=f32)
        hidden = (jax.nn.silu(gate_val) * up_val).astype(jnp.bfloat16)
        result = jnp.zeros((rows.shape[0], D), f32)
        for block in range(N_TP):
            part_sum = jnp.dot(hidden[:, block * width_block:(block + 1) * width_block], down_w[block * width_block:(block + 1) * width_block], preferred_element_type=f32)
            result = result + lax.optimization_barrier(part_sum.astype(jnp.bfloat16)).astype(f32)
        result = lax.optimization_barrier(result.astype(jnp.bfloat16)).astype(f32)
        return (total.at[index].add(weights[:, None] * result), None)
    start = jnp.zeros((TOKENS + 1, D), f32)
    total, unused = lax.scan(per_expert, start, (table, weight_table, expert_gate, expert_up, expert_down))
    return (res_float + total[:TOKENS]).astype(jnp.bfloat16)
```

```python
import functools
import jax
import jax.numpy as jnp
from jax import lax
from jax.experimental import pallas as pl
from jax.experimental.pallas import tpu as pltpu
from jax.sharding import PartitionSpec as P

epsilon = 1e-06
f32 = jnp.float32
bf16 = jnp.bfloat16
VMEM_LIMIT = 32 << 20


def shifted(value, axis, steps):
    count = lax.axis_size(axis)
    initial, last = (max(0, -steps), min(count, count - steps))
    return lax.ppermute(value, axis, [(source, source + steps) for source in range(initial, last)])


def z_shift(value, steps):
    count = lax.axis_size("tp")
    return lax.ppermute(value, "tp", [(i, (i + 2 * steps) % count) for i in range(count)])


def other_core(value):
    count = lax.axis_size("tp")
    return lax.ppermute(value, "tp", [(i, i ^ 1) for i in range(count)])


def contract_last(a, b):
    return lax.dot_general(a, b, (((1,), (1,)), ((), ())), preferred_element_type=f32)


def expert_kernel(sizes, with_token, *refs):
    count = len(sizes)
    pieces = refs[:count]
    gate_a, gate_b, up_a, up_b, down_a, down_b = refs[count : count + 6]
    at = count + 6 + with_token
    outs = refs[at : at + count]
    rows, total = refs[at + count :]
    step = pl.program_id(0)
    starts = [sum(sizes[:i]) for i in range(count)]

    @pl.when(step == 0)
    def _():
        for start, size, piece in zip(starts, sizes, pieces):
            rows[start : start + size, :] = piece[...]

    x = rows[...]
    gate_val = contract_last(x, jnp.concatenate([gate_a[...], gate_b[...]], axis=0))
    up_val = contract_last(x, jnp.concatenate([up_a[...], up_b[...]], axis=0))
    hidden = (jax.nn.silu(gate_val) * up_val).astype(bf16)
    down = jnp.concatenate([down_a[...], down_b[...]], axis=0)
    partial = jnp.dot(hidden, down, preferred_element_type=f32)

    @pl.when(step == 0)
    def _():
        total[...] = partial

    @pl.when(step > 0)
    def _():
        total[...] += partial

    @pl.when(step == pl.num_programs(0) - 1)
    def _():
        for start, size, out in zip(starts, sizes, outs):
            out[...] = total[start : start + size, :].astype(bf16)


def expert(pieces, weights, token=None, block=112):
    sizes = tuple(p.shape[0] for p in pieces)
    width = pieces[0].shape[1]
    hidden = weights[0].shape[0]
    whole = lambda size: pl.BlockSpec((size, width), lambda j: (0, 0))
    tokens = () if token is None else (token,)
    flops = 2 * 3 * sum(sizes) * width * 2 * hidden
    return pl.pallas_call(
        functools.partial(expert_kernel, sizes, len(tokens)),
        grid=(hidden // block,),
        in_specs=[whole(size) for size in sizes]
        + [pl.BlockSpec((block, width), lambda j: (j, 0))] * 6
        + [pl.BlockSpec(memory_space=pl.ANY)] * len(tokens),
        out_specs=[whole(size) for size in sizes],
        out_shape=[jax.ShapeDtypeStruct((size, width), bf16) for size in sizes],
        scratch_shapes=[
            pltpu.VMEM((sum(sizes), width), bf16),
            pltpu.VMEM((sum(sizes), width), f32),
        ],
        compiler_params=pltpu.CompilerParams(vmem_limit_bytes=VMEM_LIMIT),
        cost_estimate=pl.CostEstimate(
            flops=flops, bytes_accessed=6 * hidden * width * 2, transcendentals=0
        ),
    )(*pieces, *weights, *tokens)


def add_kernel(a, b, out):
    out[...] = (a[...].astype(f32) + b[...].astype(f32)).astype(bf16)


def add(a, b):
    return pl.pallas_call(
        add_kernel,
        out_shape=jax.ShapeDtypeStruct(a.shape, bf16),
        compiler_params=pltpu.CompilerParams(vmem_limit_bytes=8 << 20),
        cost_estimate=pl.CostEstimate(
            flops=a.size * 500, bytes_accessed=a.size * 6, transcendentals=0
        ),
    )(a, b)


def close_kernel(right_a, left_a, own_a, right_b, left_b, own_b, out):
    half = right_a.shape[0]
    out[:half, :] = (
        right_a[...].astype(f32) + left_a[...].astype(f32) + own_a[...].astype(f32)
    ).astype(bf16)
    out[half:, :] = (
        right_b[...].astype(f32) + left_b[...].astype(f32) + own_b[...].astype(f32)
    ).astype(bf16)


def close(*parts):
    half, width = parts[0].shape
    return pl.pallas_call(
        close_kernel,
        out_shape=jax.ShapeDtypeStruct((2 * half, width), bf16),
        compiler_params=pltpu.CompilerParams(vmem_limit_bytes=8 << 20),
    )(*parts)


def per_device(
    conv_value,
    conv_gate,
    conv_taps,
    norm_gain,
    norm_bias,
    out_weight,
    stream,
    routes,
    route_weights,
    expert_gain,
    expert_gate,
    expert_up,
    expert_down,
):
    local_ch = conv_value.shape[0]
    run_len = conv_value.shape[1]
    kernel_len = conv_taps.shape[1]
    gate_t = expert_gate[0].T
    up_t = expert_up[0].T
    down_w = expert_down[0]
    weights = (
        gate_t,
        other_core(gate_t),
        up_t,
        other_core(up_t),
        down_w,
        other_core(down_w),
    )

    gated_input = (conv_value.astype(f32) * jax.nn.sigmoid(conv_gate.astype(f32))).astype(bf16)
    left_rim = shifted(gated_input[:, run_len - (kernel_len - 1) :], "sp", 1)
    padded = jnp.concatenate([left_rim, gated_input], axis=1).astype(f32)
    conv_sum = jnp.zeros((local_ch, run_len), f32)
    for offset in range(kernel_len):
        conv_sum = (
            conv_sum + conv_taps[:, offset : offset + 1] * padded[:, offset : offset + run_len]
        )
    conv_out = conv_sum.astype(bf16)
    whole_conv = lax.all_to_all(conv_out, "tp", split_axis=1, concat_axis=0, tiled=True).astype(f32)
    center = jnp.mean(whole_conv, axis=0, keepdims=True)
    spread = jnp.mean((whole_conv - center) ** 2, axis=0, keepdims=True)
    scaled = (whole_conv - center) * lax.rsqrt(spread + epsilon) * norm_gain[:, None] + norm_bias[
        :, None
    ]
    token_major = jax.nn.silu(scaled).astype(bf16)
    projected = lax.dot_general(
        token_major, out_weight, (((0,), (0,)), ((), ())), preferred_element_type=f32
    )
    residual = (stream.astype(f32) + projected).astype(bf16)
    res_float = residual.astype(f32)
    normed = (
        res_float
        * lax.rsqrt(jnp.mean(res_float * res_float, axis=1, keepdims=True) + epsilon)
        * expert_gain
    ).astype(bf16)
    tok_rows = stream.shape[0]
    width = stream.shape[1]
    top_count = routes.shape[1]
    experts = lax.axis_size("sp")
    capacity = top_count * tok_rows // experts
    flat_ids = routes.reshape(-1)
    onehot = (flat_ids[:, None] == jnp.arange(experts, dtype=jnp.int32)[None, :]).astype(jnp.int32)
    before = jnp.cumsum(onehot, axis=0) - onehot
    rank = jnp.sum(before * onehot, axis=1)
    slots = (flat_ids * capacity + rank).reshape(tok_rows, top_count)
    slot_ids = jnp.arange(experts * capacity, dtype=jnp.int32)
    chooser = jnp.any(slots[None, :, :] == slot_ids[:, None, None], axis=2).astype(bf16)
    send_rows = (
        jnp.dot(chooser, normed, preferred_element_type=f32)
        .astype(bf16)
        .reshape(experts, capacity, width)
    )
    received = lax.all_to_all(send_rows, "sp", split_axis=0, concat_axis=0, tiled=True)
    received, weights = lax.optimization_barrier((received, weights))
    own = received.reshape(-1, width)

    far = lax.axis_size("tp") // 4
    half = own.shape[0] // 2
    from_left = {0: (own[:half], own[half:])}
    from_right = {0: from_left[0]}
    for k in range(1, far + 1):
        left_a, left_b = from_left[k - 1]
        right_a, right_b = from_right[k - 1]
        from_left[k] = (z_shift(left_a, 1), z_shift(left_b, 1) if k < far else None)
        from_right[k] = (z_shift(right_a, -1) if k < far else None, z_shift(right_b, -1))

    first = expert((*from_left[0], *from_left[1], *from_right[1]), weights)
    part_own = first[0:2]
    part_left, part_right = {1: first[2:4]}, {1: first[4:6]}
    token = first[0]
    for k in range(2, far):
        parts = expert((*from_left[k], *from_right[k]), weights, token)
        part_left[k], part_right[k] = parts[0:2], parts[2:4]
        token = parts[0]
    antipode = expert((from_left[far][0], from_right[far][1]), weights, token)

    right_a, left_b = z_shift(antipode[0], 1), z_shift(antipode[1], -1)
    right_b, left_a = None, None
    for k in range(far - 1, 0, -1):
        out_rb = part_right[k][1] if right_b is None else add(right_b, part_right[k][1])
        out_la = part_left[k][0] if left_a is None else add(left_a, part_left[k][0])
        right_b, left_a = z_shift(out_rb, 1), z_shift(out_la, -1)
        right_a = z_shift(add(right_a, part_right[k][0]), 1)
        left_b = z_shift(add(left_b, part_left[k][1]), -1)
    result = close(right_a, left_a, part_own[0], right_b, left_b, part_own[1])
    result = result.reshape(received.shape)
    returned = lax.all_to_all(result, "sp", split_axis=0, concat_axis=0, tiled=True)
    weight_hi = route_weights.astype(bf16).astype(f32)
    weight_lo = route_weights - weight_hi

    def spread_weights(weight):
        hit = slots[:, :, None] == slot_ids[None, None, :]
        return jnp.sum(jnp.where(hit, weight[:, :, None], 0.0), axis=1).astype(bf16)

    rows = returned.reshape(experts * capacity, width)
    expert_sum = jnp.dot(
        spread_weights(weight_hi), rows, preferred_element_type=f32
    ) + jnp.dot(spread_weights(weight_lo), rows, preferred_element_type=f32)
    return (res_float + expert_sum).astype(bf16)


def solution(mesh):
    return jax.shard_map(
        per_device,
        mesh=mesh,
        in_specs=(
            P("tp", "sp"),
            P("tp", "sp"),
            P("tp", None),
            P(),
            P(),
            P(),
            P(("sp", "tp"), None),
            P(("sp", "tp"), None),
            P(("sp", "tp"), None),
            P(),
            P("sp", None, "tp"),
            P("sp", None, "tp"),
            P("sp", "tp", None),
        ),
        out_specs=P(("sp", "tp"), None),
        check_vma=False,
    )
```

```python
import functools
import jax
import jax.numpy as jnp
from jax import lax
from jax.experimental import pallas as pl
from jax.experimental.pallas import tpu as pltpu
from jax.sharding import PartitionSpec as P

epsilon = 1e-06
f32 = jnp.float32
bf16 = jnp.bfloat16
VMEM_LIMIT = 12 << 20
TILE = 128
EXPERTS = 16


def shifted(value, axis, steps):
    count = lax.axis_size(axis)
    initial, last = (max(0, -steps), min(count, count - steps))
    return lax.ppermute(value, axis, [(source, source + steps) for source in range(initial, last)])


def z_shift(value, steps):
    count = lax.axis_size("tp")
    return lax.ppermute(value, "tp", [(i, (i + 2 * steps) % count) for i in range(count)])


def other_core(value):
    count = lax.axis_size("tp")
    return lax.ppermute(value, "tp", [(i, i ^ 1) for i in range(count)])


def contract_last(a, b):
    return lax.dot_general(a, b, (((1,), (1,)), ((), ())), preferred_element_type=f32)


def expert_kernel(sizes, block, with_token, *refs):
    count = len(sizes)
    pieces = refs[:count]
    gate_a, gate_b, up_a, up_b, down_a, down_b = refs[count : count + 6]
    at = count + 6 + with_token
    outs = refs[at : at + count]
    rows, total = refs[at + count :]
    starts = [sum(sizes[:i]) for i in range(count)]
    for start, size, piece in zip(starts, sizes, pieces):
        rows[start : start + size, :] = piece[...]
    x = rows[...]

    def partial(step):
        at = pl.ds(pl.multiple_of(step * block, block), block)
        both = lambda a, b: jnp.concatenate([a[at, :], b[at, :]], axis=0)
        gate_val = contract_last(x, both(gate_a, gate_b))
        up_val = contract_last(x, both(up_a, up_b))
        hidden = (jax.nn.silu(gate_val) * up_val).astype(bf16)
        return jnp.dot(hidden, both(down_a, down_b), preferred_element_type=f32)

    total[...] = jnp.zeros_like(total)

    @pl.loop(0, gate_a.shape[0] // block)
    def _(step):
        total[...] += partial(step)

    for start, size, out in zip(starts, sizes, outs):
        out[...] = total[start : start + size, :].astype(bf16)


def in_vmem(count):
    return [pl.BlockSpec(memory_space=pltpu.VMEM)] * count


def expert(pieces, weights, token=None):
    sizes = tuple(p.shape[0] for p in pieces)
    width = pieces[0].shape[1]
    hidden = weights[0].shape[0]
    tokens = () if token is None else (token,)
    flops = 2 * 3 * sum(sizes) * width * 2 * hidden
    return pl.pallas_call(
        functools.partial(expert_kernel, sizes, hidden // 2, len(tokens)),
        in_specs=in_vmem(len(sizes) + 6) + [pl.BlockSpec(memory_space=pl.ANY)] * len(tokens),
        out_specs=in_vmem(len(sizes)),
        out_shape=[jax.ShapeDtypeStruct((size, width), bf16) for size in sizes],
        scratch_shapes=[
            pltpu.VMEM((sum(sizes), width), bf16),
            pltpu.VMEM((sum(sizes), width), f32),
        ],
        compiler_params=pltpu.CompilerParams(vmem_limit_bytes=VMEM_LIMIT),
        cost_estimate=pl.CostEstimate(flops=flops, bytes_accessed=1 << 20, transcendentals=0),
    )(*pieces, *weights, *tokens)


def gated(value, gate):
    value, gate = value.astype(f32), gate.astype(f32)
    return (value * jax.nn.sigmoid(gate)).astype(bf16)


def position_major(lanes):
    pair = TILE // 4
    last = lanes.shape[1] - TILE
    here = lanes[:, :last]
    ahead = jnp.concatenate([lanes[:, pair:last], lanes[:, last : last + pair]], axis=1)
    return jnp.concatenate([here, ahead], axis=0).T


def tap_sum(laid, start, rows, taps):
    count = taps.shape[0]
    total = jnp.zeros((rows, laid.shape[1]), f32)
    for j in range(count):
        total = total + taps[j : j + 1, :] * laid[start + j : start + j + rows, :]
    return total.astype(bf16)


def twice(taps):
    return jnp.concatenate([taps[...], taps[...]], axis=1)


def conv_main_kernel(far_value, far_gate, far_taps, out, laid, value, gate, taps, arrived):
    pairs = ((far_value, value), (far_gate, gate), (far_taps, taps))
    fetches = [pltpu.make_async_copy(*pair, arrived.at[i]) for i, pair in enumerate(pairs)]
    for fetch in fetches:
        fetch.start()
    for fetch in fetches:
        fetch.wait()
    blocks, rows, _ = out.shape
    both = twice(taps)
    line = gated(value[...], gate[...]).astype(f32)
    line = jnp.concatenate([line, jnp.zeros((line.shape[0], TILE), f32)], axis=1)
    laid[...] = position_major(line)
    lead = both.shape[0] - 1

    @pl.loop(1, blocks)
    def _(block):
        window = laid[pl.ds(pl.multiple_of(2 * rows * (block - 1) + rows, rows), 2 * rows), :]
        out[block, :, :] = tap_sum(window, rows - lead, rows, both)


def conv_first_kernel(rim, value, gate, taps, _, out, laid):
    rows = out.shape[1]
    both = twice(taps)
    line = gated(value[...], gate[...]).astype(f32)
    line = jnp.concatenate([rim[...].astype(f32), line, jnp.zeros_like(line)], axis=1)
    laid[...] = position_major(line)
    lead = both.shape[0] - 1
    out[0, :, :] = tap_sum(laid, rim.shape[1] - lead, rows, both)


def convolve(conv_value, conv_gate, taps, rim, blocks):
    channels, length = conv_value.shape
    rows = length // blocks // 2
    shape = jax.ShapeDtypeStruct((blocks, rows, 2 * channels), bf16)
    main = pl.pallas_call(
        conv_main_kernel,
        in_specs=[pl.BlockSpec(memory_space=pltpu.HBM)] * 3,
        out_specs=in_vmem(1)[0],
        out_shape=shape,
        scratch_shapes=[
            pltpu.VMEM((length, 2 * channels), f32),
            pltpu.VMEM(conv_value.shape, bf16),
            pltpu.VMEM(conv_gate.shape, bf16),
            pltpu.VMEM(taps.shape, f32),
            pltpu.SemaphoreType.DMA((3,)),
        ],
        compiler_params=pltpu.CompilerParams(vmem_limit_bytes=4 << 20),
        cost_estimate=pl.CostEstimate(flops=5 << 28, bytes_accessed=1 << 20, transcendentals=0),
    )(conv_value, conv_gate, taps)
    return pl.pallas_call(
        conv_first_kernel,
        grid=(1,),
        in_specs=[
            pl.BlockSpec(rim.shape, lambda i: (0, 0)),
            pl.BlockSpec((channels, TILE), lambda i: (0, 0)),
            pl.BlockSpec((channels, TILE), lambda i: (0, 0)),
            pl.BlockSpec(taps.shape, lambda i: (0, 0)),
            pl.BlockSpec(memory_space=pl.ANY),
        ],
        out_specs=pl.BlockSpec((1, rows, 2 * channels), lambda i: (0, 0, 0)),
        out_shape=shape,
        scratch_shapes=[pltpu.VMEM((rim.shape[1] + TILE, 2 * channels), f32)],
        input_output_aliases={4: 0},
        compiler_params=pltpu.CompilerParams(vmem_limit_bytes=4 << 20),
        cost_estimate=pl.CostEstimate(flops=1 << 27, bytes_accessed=1 << 16, transcendentals=0),
    )(rim, conv_value, conv_gate, taps, main)


def token_kernel(
    conv,
    gain,
    bias,
    out_weight,
    stream,
    expert_gain,
    routes,
    route_weights,
    send,
    residual,
    mixer_hi,
    mixer_lo,
):
    top, tokens = routes.shape
    slot_count = send.shape[0]
    capacity = slot_count // EXPERTS
    names = lax.broadcasted_iota(jnp.int32, (EXPERTS, tokens), 0)
    hits = [(names == routes[k : k + 1, :]).astype(f32) for k in range(top)]
    earlier = lax.broadcasted_iota(jnp.int32, (tokens, tokens), 0) < lax.broadcasted_iota(
        jnp.int32, (tokens, tokens), 1
    )
    before = jnp.dot(
        sum(hits).astype(bf16), earlier.astype(bf16), preferred_element_type=f32
    )
    places = lax.broadcasted_iota(jnp.int32, (slot_count, tokens), 0)
    chooser = jnp.zeros((slot_count, tokens), f32)
    weighted = jnp.zeros((slot_count, tokens), f32)
    for k in range(top):
        rank = jnp.sum(before * hits[k], axis=0, keepdims=True).astype(jnp.int32)
        taken = places == routes[k : k + 1, :] * capacity + rank
        chooser = chooser + jnp.where(taken, 1.0, 0.0)
        weighted = weighted + jnp.where(taken, route_weights[k : k + 1, :], 0.0)
        before = before + hits[k]
    upper = weighted.astype(bf16)
    mixer_hi[...] = upper
    mixer_lo[...] = (weighted - upper.astype(f32)).astype(bf16)

    parts, _, lanes = conv.shape
    half = lanes // 2
    x = jnp.concatenate(
        [
            jnp.concatenate([conv[p, :, :half] for p in range(parts)], axis=1),
            jnp.concatenate([conv[p, :, half:] for p in range(parts)], axis=1),
        ],
        axis=0,
    ).astype(f32)
    center = jnp.mean(x, axis=1, keepdims=True)
    x = x - center
    spread = jnp.mean(x * x, axis=1, keepdims=True)
    scaled = x * lax.rsqrt(spread + epsilon) * gain[...] + bias[...]
    active = jax.nn.silu(scaled).astype(bf16)
    projected = jnp.dot(active, out_weight[...], preferred_element_type=f32)
    kept = (stream[...].astype(f32) + projected).astype(bf16)
    residual[...] = kept
    kept = kept.astype(f32)
    scale = lax.rsqrt(jnp.mean(kept * kept, axis=1, keepdims=True) + epsilon)
    normed = (kept * scale * expert_gain[...]).astype(bf16)
    send[...] = jnp.dot(chooser.astype(bf16), normed, preferred_element_type=f32).astype(bf16)


def token_block(conv, gain, bias, out_weight, stream, expert_gain, routes, route_weights):
    top, tokens = routes.shape
    return pl.pallas_call(
        token_kernel,
        in_specs=in_vmem(8),
        out_specs=in_vmem(4),
        out_shape=[
            jax.ShapeDtypeStruct((top * tokens, stream.shape[1]), bf16),
            jax.ShapeDtypeStruct(stream.shape, bf16),
            jax.ShapeDtypeStruct((top * tokens, tokens), bf16),
            jax.ShapeDtypeStruct((top * tokens, tokens), bf16),
        ],
        compiler_params=pltpu.CompilerParams(vmem_limit_bytes=12 << 20),
        cost_estimate=pl.CostEstimate(flops=3 << 29, bytes_accessed=5 << 20, transcendentals=0),
    )(
        conv,
        gain[None, :],
        bias[None, :],
        out_weight,
        stream,
        expert_gain[None, :],
        routes,
        route_weights,
    )


def add_kernel(a, b, out):
    out[...] = (a[...].astype(f32) + b[...].astype(f32)).astype(bf16)


def add(a, b):
    return pl.pallas_call(
        add_kernel,
        out_shape=jax.ShapeDtypeStruct(a.shape, bf16),
        compiler_params=pltpu.CompilerParams(vmem_limit_bytes=4 << 20),
        cost_estimate=pl.CostEstimate(
            flops=a.size * 500, bytes_accessed=a.size * 6, transcendentals=0
        ),
    )(a, b)


def split_kernel(both, first, second):
    half = first.shape[0]
    first[...] = both[:half, :]
    second[...] = both[half:, :]


def split(both):
    half = jax.ShapeDtypeStruct((both.shape[0] // 2, both.shape[1]), both.dtype)
    return pl.pallas_call(
        split_kernel,
        in_specs=in_vmem(1),
        out_specs=in_vmem(2),
        out_shape=[half, half],
        compiler_params=pltpu.CompilerParams(vmem_limit_bytes=4 << 20),
    )(both)


def close_kernel(right_a, left_a, own_a, right_b, left_b, own_b, out):
    half = right_a.shape[0]
    out[:half, :] = (
        right_a[...].astype(f32) + left_a[...].astype(f32) + own_a[...].astype(f32)
    ).astype(bf16)
    out[half:, :] = (
        right_b[...].astype(f32) + left_b[...].astype(f32) + own_b[...].astype(f32)
    ).astype(bf16)


def close(*parts):
    half, width = parts[0].shape
    return pl.pallas_call(
        close_kernel,
        out_shape=jax.ShapeDtypeStruct((2 * half, width), bf16),
        compiler_params=pltpu.CompilerParams(vmem_limit_bytes=4 << 20),
    )(*parts)


def per_device(
    conv_value,
    conv_gate,
    conv_taps,
    norm_gain,
    norm_bias,
    out_weight,
    stream,
    routes,
    route_weights,
    expert_gain,
    expert_gate,
    expert_up,
    expert_down,
):
    run_len = conv_value.shape[1]
    rim = gated(conv_value[:, run_len - TILE :], conv_gate[:, run_len - TILE :])
    rim = shifted(rim, "sp", 1)
    blocks = lax.axis_size("tp")
    conv_out = convolve(conv_value, conv_gate, conv_taps.T, rim, blocks)
    tok_rows = stream.shape[0]
    width = stream.shape[1]
    top_count = routes.shape[1]
    experts = lax.axis_size("sp")
    capacity = top_count * tok_rows // experts
    whole_conv = lax.all_to_all(conv_out, "tp", split_axis=0, concat_axis=0, tiled=True)
    send_rows, residual, mixer_hi, mixer_lo = token_block(
        whole_conv,
        norm_gain,
        norm_bias,
        out_weight,
        stream,
        expert_gain,
        routes.T,
        route_weights.T,
    )
    mine = (expert_gate[0].T, expert_up[0].T, expert_down[0])
    send_rows, gone = lax.optimization_barrier((send_rows, mine))
    weights = [w for pair in zip(mine, map(other_core, gone)) for w in pair]
    send_rows = send_rows.reshape(experts, capacity, width)
    received = lax.all_to_all(send_rows, "sp", split_axis=0, concat_axis=0, tiled=True)
    received, weights = lax.optimization_barrier((received, weights))
    own = received.reshape(-1, width)

    far = lax.axis_size("tp") // 4
    from_left = {0: tuple(split(own))}
    from_right = {0: from_left[0]}
    for k in range(1, far + 1):
        left_a, left_b = from_left[k - 1]
        right_a, right_b = from_right[k - 1]
        from_left[k] = (z_shift(left_a, 1), z_shift(left_b, 1) if k < far else None)
        from_right[k] = (z_shift(right_a, -1) if k < far else None, z_shift(right_b, -1))

    first = expert((*from_left[0], *from_left[1], *from_right[1]), weights)
    part_own = first[0:2]
    part_left, part_right = {1: first[2:4]}, {1: first[4:6]}
    token = first[0]
    for k in range(2, far):
        parts = expert((*from_left[k], *from_right[k]), weights, token)
        part_left[k], part_right[k] = parts[0:2], parts[2:4]
        token = parts[0]
    right_b = z_shift(part_right[far - 1][1], 1)
    left_a = z_shift(part_left[far - 1][0], -1)
    antipode = expert((from_left[far][0], from_right[far][1]), weights, token)

    right_a, left_b = z_shift(antipode[0], 1), z_shift(antipode[1], -1)
    for k in range(far - 1, 0, -1):
        if k < far - 1:
            right_b = z_shift(add(right_b, part_right[k][1]), 1)
            left_a = z_shift(add(left_a, part_left[k][0]), -1)
        right_a = z_shift(add(right_a, part_right[k][0]), 1)
        left_b = z_shift(add(left_b, part_left[k][1]), -1)
    result = close(right_a, left_a, part_own[0], right_b, left_b, part_own[1])
    result = result.reshape(received.shape)
    returned = lax.all_to_all(result, "sp", split_axis=0, concat_axis=0, tiled=True)
    rows = returned.reshape(experts * capacity, width)

    def mix(weight):
        return lax.dot_general(weight, rows, (((0,), (0,)), ((), ())), preferred_element_type=f32)

    expert_sum = mix(mixer_hi) + mix(mixer_lo)
    return (residual.astype(f32) + expert_sum).astype(bf16)


def solution(mesh):
    return jax.shard_map(
        per_device,
        mesh=mesh,
        in_specs=(
            P("tp", "sp"),
            P("tp", "sp"),
            P("tp", None),
            P(),
            P(),
            P(),
            P(("sp", "tp"), None),
            P(("sp", "tp"), None),
            P(("sp", "tp"), None),
            P(),
            P("sp", None, "tp"),
            P("sp", None, "tp"),
            P("sp", "tp", None),
        ),
        out_specs=P(("sp", "tp"), None),
        check_vma=False,
    )
```

```python
import functools
import jax
import jax.numpy as jnp
from jax import lax
from jax.experimental import pallas as pl
from jax.experimental.pallas import tpu as pltpu
from jax.sharding import PartitionSpec as P

epsilon = 1e-06
f32 = jnp.float32
bf16 = jnp.bfloat16
VMEM_LIMIT = 12 << 20
TILE = 128
EXPERTS = 16


def shifted(value, axis, steps):
    count = lax.axis_size(axis)
    initial, last = (max(0, -steps), min(count, count - steps))
    return lax.ppermute(value, axis, [(source, source + steps) for source in range(initial, last)])


def z_shift(value, steps):
    count = lax.axis_size("tp")
    return lax.ppermute(value, "tp", [(i, (i + 2 * steps) % count) for i in range(count)])


def other_core(value):
    count = lax.axis_size("tp")
    return lax.ppermute(value, "tp", [(i, i ^ 1) for i in range(count)])


def contract_last(a, b):
    return lax.dot_general(a, b, (((1,), (1,)), ((), ())), preferred_element_type=f32)


def expert_kernel(sizes, block, with_token, *refs):
    count = len(sizes)
    pieces = refs[:count]
    gate_a, gate_b, up_a, up_b, down_a, down_b = refs[count : count + 6]
    at = count + 6 + with_token
    outs = refs[at : at + count]
    rows, total = refs[at + count :]
    starts = [sum(sizes[:i]) for i in range(count)]
    for start, size, piece in zip(starts, sizes, pieces):
        rows[start : start + size, :] = piece[...]
    x = rows[...]

    def partial(step):
        at = pl.ds(pl.multiple_of(step * block, block), block)
        both = lambda a, b: jnp.concatenate([a[at, :], b[at, :]], axis=0)
        gate_val = contract_last(x, both(gate_a, gate_b))
        up_val = contract_last(x, both(up_a, up_b))
        hidden = (jax.nn.silu(gate_val) * up_val).astype(bf16)
        return jnp.dot(hidden, both(down_a, down_b), preferred_element_type=f32)

    total[...] = jnp.zeros_like(total)

    @pl.loop(0, gate_a.shape[0] // block)
    def _(step):
        total[...] += partial(step)

    for start, size, out in zip(starts, sizes, outs):
        out[...] = total[start : start + size, :].astype(bf16)


def in_vmem(count):
    return [pl.BlockSpec(memory_space=pltpu.VMEM)] * count


def expert(pieces, weights, token=None):
    sizes = tuple(p.shape[0] for p in pieces)
    width = pieces[0].shape[1]
    hidden = weights[0].shape[0]
    tokens = () if token is None else (token,)
    flops = 2 * 3 * sum(sizes) * width * 2 * hidden
    return pl.pallas_call(
        functools.partial(expert_kernel, sizes, hidden // 2, len(tokens)),
        in_specs=in_vmem(len(sizes) + 6) + [pl.BlockSpec(memory_space=pl.ANY)] * len(tokens),
        out_specs=in_vmem(len(sizes)),
        out_shape=[jax.ShapeDtypeStruct((size, width), bf16) for size in sizes],
        scratch_shapes=[
            pltpu.VMEM((sum(sizes), width), bf16),
            pltpu.VMEM((sum(sizes), width), f32),
        ],
        compiler_params=pltpu.CompilerParams(vmem_limit_bytes=VMEM_LIMIT),
        cost_estimate=pl.CostEstimate(flops=flops, bytes_accessed=1 << 20, transcendentals=0),
    )(*pieces, *weights, *tokens)


def gated(value, gate):
    value, gate = value.astype(f32), gate.astype(f32)
    return (value * jax.nn.sigmoid(gate)).astype(bf16)


def position_major(lanes):
    pair = TILE // 4
    last = lanes.shape[1] - TILE
    here = lanes[:, :last]
    ahead = jnp.concatenate([lanes[:, pair:last], lanes[:, last : last + pair]], axis=1)
    return jnp.concatenate([here, ahead], axis=0).T


def tap_sum(laid, start, rows, taps):
    count = taps.shape[0]
    total = jnp.zeros((rows, laid.shape[1]), f32)
    for j in range(count):
        total = total + taps[j : j + 1, :] * laid[start + j : start + j + rows, :]
    return total.astype(bf16)


def twice(taps):
    return jnp.concatenate([taps[...], taps[...]], axis=1)


def conv_main_kernel(far_value, far_gate, far_taps, out, laid, value, gate, taps, arrived):
    pairs = ((far_value, value), (far_gate, gate), (far_taps, taps))
    fetches = [pltpu.make_async_copy(*pair, arrived.at[i]) for i, pair in enumerate(pairs)]
    for fetch in fetches:
        fetch.start()
    for fetch in fetches:
        fetch.wait()
    blocks, rows, _ = out.shape
    both = twice(taps)
    line = gated(value[...], gate[...]).astype(f32)
    line = jnp.concatenate([line, jnp.zeros((line.shape[0], TILE), f32)], axis=1)
    laid[...] = position_major(line)
    lead = both.shape[0] - 1

    @pl.loop(1, blocks)
    def _(block):
        window = laid[pl.ds(pl.multiple_of(2 * rows * (block - 1) + rows, rows), 2 * rows), :]
        out[block, :, :] = tap_sum(window, rows - lead, rows, both)


def conv_first_kernel(rim, value, gate, taps, _, out, laid):
    rows = out.shape[1]
    both = twice(taps)
    line = gated(value[...], gate[...]).astype(f32)
    line = jnp.concatenate([rim[...].astype(f32), line, jnp.zeros_like(line)], axis=1)
    laid[...] = position_major(line)
    lead = both.shape[0] - 1
    out[0, :, :] = tap_sum(laid, rim.shape[1] - lead, rows, both)


def convolve(conv_value, conv_gate, taps, rim, blocks):
    channels, length = conv_value.shape
    rows = length // blocks // 2
    shape = jax.ShapeDtypeStruct((blocks, rows, 2 * channels), bf16)
    main = pl.pallas_call(
        conv_main_kernel,
        in_specs=[pl.BlockSpec(memory_space=pltpu.HBM)] * 3,
        out_specs=in_vmem(1)[0],
        out_shape=shape,
        scratch_shapes=[
            pltpu.VMEM((length, 2 * channels), f32),
            pltpu.VMEM(conv_value.shape, bf16),
            pltpu.VMEM(conv_gate.shape, bf16),
            pltpu.VMEM(taps.shape, f32),
            pltpu.SemaphoreType.DMA((3,)),
        ],
        compiler_params=pltpu.CompilerParams(vmem_limit_bytes=4 << 20),
        cost_estimate=pl.CostEstimate(flops=5 << 28, bytes_accessed=1 << 20, transcendentals=0),
    )(conv_value, conv_gate, taps)
    return pl.pallas_call(
        conv_first_kernel,
        grid=(1,),
        in_specs=[
            pl.BlockSpec(rim.shape, lambda i: (0, 0)),
            pl.BlockSpec((channels, TILE), lambda i: (0, 0)),
            pl.BlockSpec((channels, TILE), lambda i: (0, 0)),
            pl.BlockSpec(taps.shape, lambda i: (0, 0)),
            pl.BlockSpec(memory_space=pl.ANY),
        ],
        out_specs=pl.BlockSpec((1, rows, 2 * channels), lambda i: (0, 0, 0)),
        out_shape=shape,
        scratch_shapes=[pltpu.VMEM((rim.shape[1] + TILE, 2 * channels), f32)],
        input_output_aliases={4: 0},
        compiler_params=pltpu.CompilerParams(vmem_limit_bytes=4 << 20),
        cost_estimate=pl.CostEstimate(flops=1 << 27, bytes_accessed=1 << 16, transcendentals=0),
    )(rim, conv_value, conv_gate, taps, main)


def token_kernel(
    conv,
    gain,
    bias,
    out_weight,
    stream,
    expert_gain,
    routes,
    route_weights,
    send,
    residual,
    mixer_hi,
    mixer_lo,
):
    top, tokens = routes.shape
    slot_count = send.shape[0]
    capacity = slot_count // EXPERTS
    names = lax.broadcasted_iota(jnp.int32, (EXPERTS, tokens), 0)
    hits = [(names == routes[k : k + 1, :]).astype(f32) for k in range(top)]
    earlier = lax.broadcasted_iota(jnp.int32, (tokens, tokens), 0) < lax.broadcasted_iota(
        jnp.int32, (tokens, tokens), 1
    )
    before = jnp.dot(
        sum(hits).astype(bf16), earlier.astype(bf16), preferred_element_type=f32
    )
    places = lax.broadcasted_iota(jnp.int32, (slot_count, tokens), 0)
    chooser = jnp.zeros((slot_count, tokens), f32)
    weighted = jnp.zeros((slot_count, tokens), f32)
    for k in range(top):
        rank = jnp.sum(before * hits[k], axis=0, keepdims=True).astype(jnp.int32)
        taken = places == routes[k : k + 1, :] * capacity + rank
        chooser = chooser + jnp.where(taken, 1.0, 0.0)
        weighted = weighted + jnp.where(taken, route_weights[k : k + 1, :], 0.0)
        before = before + hits[k]
    upper = weighted.astype(bf16)
    mixer_hi[...] = upper
    mixer_lo[...] = (weighted - upper.astype(f32)).astype(bf16)

    parts, _, lanes = conv.shape
    half = lanes // 2
    x = jnp.concatenate(
        [
            jnp.concatenate([conv[p, :, :half] for p in range(parts)], axis=1),
            jnp.concatenate([conv[p, :, half:] for p in range(parts)], axis=1),
        ],
        axis=0,
    ).astype(f32)
    center = jnp.mean(x, axis=1, keepdims=True)
    x = x - center
    spread = jnp.mean(x * x, axis=1, keepdims=True)
    scaled = x * lax.rsqrt(spread + epsilon) * gain[...] + bias[...]
    active = jax.nn.silu(scaled).astype(bf16)
    projected = jnp.dot(active, out_weight[...], preferred_element_type=f32)
    kept = (stream[...].astype(f32) + projected).astype(bf16)
    residual[...] = kept
    kept = kept.astype(f32)
    scale = lax.rsqrt(jnp.mean(kept * kept, axis=1, keepdims=True) + epsilon)
    normed = (kept * scale * expert_gain[...]).astype(bf16)
    send[...] = jnp.dot(chooser.astype(bf16), normed, preferred_element_type=f32).astype(bf16)


def token_block(conv, gain, bias, out_weight, stream, expert_gain, routes, route_weights):
    top, tokens = routes.shape
    return pl.pallas_call(
        token_kernel,
        in_specs=in_vmem(8),
        out_specs=in_vmem(4),
        out_shape=[
            jax.ShapeDtypeStruct((top * tokens, stream.shape[1]), bf16),
            jax.ShapeDtypeStruct(stream.shape, bf16),
            jax.ShapeDtypeStruct((top * tokens, tokens), bf16),
            jax.ShapeDtypeStruct((top * tokens, tokens), bf16),
        ],
        compiler_params=pltpu.CompilerParams(vmem_limit_bytes=12 << 20),
        cost_estimate=pl.CostEstimate(flops=3 << 29, bytes_accessed=5 << 20, transcendentals=0),
    )(
        conv,
        gain[None, :],
        bias[None, :],
        out_weight,
        stream,
        expert_gain[None, :],
        routes,
        route_weights,
    )


def add_kernel(a, b, out):
    out[...] = (a[...].astype(f32) + b[...].astype(f32)).astype(bf16)


def add(a, b):
    return pl.pallas_call(
        add_kernel,
        out_shape=jax.ShapeDtypeStruct(a.shape, bf16),
        compiler_params=pltpu.CompilerParams(vmem_limit_bytes=4 << 20),
        cost_estimate=pl.CostEstimate(
            flops=a.size * 500, bytes_accessed=a.size * 6, transcendentals=0
        ),
    )(a, b)


def split_kernel(both, first, second):
    half = first.shape[0]
    first[...] = both[:half, :]
    second[...] = both[half:, :]


def split(both):
    half = jax.ShapeDtypeStruct((both.shape[0] // 2, both.shape[1]), both.dtype)
    return pl.pallas_call(
        split_kernel,
        in_specs=in_vmem(1),
        out_specs=in_vmem(2),
        out_shape=[half, half],
        compiler_params=pltpu.CompilerParams(vmem_limit_bytes=4 << 20),
    )(both)


def close_kernel(right_a, left_a, own_a, right_b, left_b, own_b, out):
    half = right_a.shape[0]
    out[:half, :] = (
        right_a[...].astype(f32) + left_a[...].astype(f32) + own_a[...].astype(f32)
    ).astype(bf16)
    out[half:, :] = (
        right_b[...].astype(f32) + left_b[...].astype(f32) + own_b[...].astype(f32)
    ).astype(bf16)


def close(*parts):
    half, width = parts[0].shape
    return pl.pallas_call(
        close_kernel,
        out_shape=jax.ShapeDtypeStruct((2 * half, width), bf16),
        compiler_params=pltpu.CompilerParams(vmem_limit_bytes=4 << 20),
    )(*parts)


def per_device(
    conv_value,
    conv_gate,
    conv_taps,
    norm_gain,
    norm_bias,
    out_weight,
    stream,
    routes,
    route_weights,
    expert_gain,
    expert_gate,
    expert_up,
    expert_down,
):
    run_len = conv_value.shape[1]
    rim = gated(conv_value[:, run_len - TILE :], conv_gate[:, run_len - TILE :])
    rim = shifted(rim, "sp", 1)
    blocks = lax.axis_size("tp")
    conv_out = convolve(conv_value, conv_gate, conv_taps.T, rim, blocks)
    tok_rows = stream.shape[0]
    width = stream.shape[1]
    top_count = routes.shape[1]
    experts = lax.axis_size("sp")
    capacity = top_count * tok_rows // experts
    whole_conv = lax.all_to_all(conv_out, "tp", split_axis=0, concat_axis=0, tiled=True)
    send_rows, residual, mixer_hi, mixer_lo = token_block(
        whole_conv,
        norm_gain,
        norm_bias,
        out_weight,
        stream,
        expert_gain,
        routes.T,
        route_weights.T,
    )
    mine = (expert_gate[0].T, expert_up[0].T, expert_down[0])
    send_rows, gone = lax.optimization_barrier((send_rows, mine))
    weights = [w for pair in zip(mine, map(other_core, gone)) for w in pair]
    send_rows = send_rows.reshape(experts, capacity, width)
    received = lax.all_to_all(send_rows, "sp", split_axis=0, concat_axis=0, tiled=True)
    received, weights = lax.optimization_barrier((received, weights))
    own = received.reshape(-1, width)

    far = lax.axis_size("tp") // 4
    from_left = {0: tuple(split(own))}
    from_right = {0: from_left[0]}
    for k in range(1, far + 1):
        left_a, left_b = from_left[k - 1]
        right_a, right_b = from_right[k - 1]
        left_a = z_shift(left_a, 1)
        right_b = z_shift(right_b, -1)
        left_b = z_shift(left_b, 1) if k < far else None
        right_a = z_shift(right_a, -1) if k < far else None
        from_left[k] = (left_a, left_b)
        from_right[k] = (right_a, right_b)

    part_own = expert(from_left[0], weights)
    part_left, part_right = {}, {}
    token = part_own[0]
    for k in range(2, far):
        parts = expert((*from_left[k], *from_right[k]), weights, token)
        part_left[k], part_right[k] = parts[0:2], parts[2:4]
        token = parts[0]
    right_b = z_shift(part_right[far - 1][1], 1)
    left_a = z_shift(part_left[far - 1][0], -1)
    antipode = expert((from_left[far][0], from_right[far][1]), weights, token)

    right_a = z_shift(antipode[0], 1)
    left_b = z_shift(antipode[1], -1)
    parts = expert((*from_left[1], *from_right[1]), weights, antipode[0])
    part_left[1], part_right[1] = parts[0:2], parts[2:4]
    for k in range(far - 1, 0, -1):
        if k < far - 1:
            right_b = z_shift(add(right_b, part_right[k][1]), 1)
            left_a = z_shift(add(left_a, part_left[k][0]), -1)
        right_a = z_shift(add(right_a, part_right[k][0]), 1)
        left_b = z_shift(add(left_b, part_left[k][1]), -1)
    result = close(right_a, left_a, part_own[0], right_b, left_b, part_own[1])
    result = result.reshape(received.shape)
    returned = lax.all_to_all(result, "sp", split_axis=0, concat_axis=0, tiled=True)
    rows = returned.reshape(experts * capacity, width)

    def mix(weight):
        return lax.dot_general(weight, rows, (((0,), (0,)), ((), ())), preferred_element_type=f32)

    expert_sum = mix(mixer_hi) + mix(mixer_lo)
    return (residual.astype(f32) + expert_sum).astype(bf16)


def solution(mesh):
    return jax.shard_map(
        per_device,
        mesh=mesh,
        in_specs=(
            P("tp", "sp"),
            P("tp", "sp"),
            P("tp", None),
            P(),
            P(),
            P(),
            P(("sp", "tp"), None),
            P(("sp", "tp"), None),
            P(("sp", "tp"), None),
            P(),
            P("sp", None, "tp"),
            P("sp", None, "tp"),
            P("sp", "tp", None),
        ),
        out_specs=P(("sp", "tp"), None),
        check_vma=False,
    )
```

```python
import functools
import jax
import jax.numpy as jnp
from jax import lax
from jax.experimental import pallas as pl
from jax.experimental.pallas import tpu as pltpu
from jax.sharding import PartitionSpec as P

epsilon = 1e-06
f32 = jnp.float32
bf16 = jnp.bfloat16
VMEM_LIMIT = 12 << 20
TILE = 128
EXPERTS = 16


def shifted(value, axis, steps):
    count = lax.axis_size(axis)
    initial, last = (max(0, -steps), min(count, count - steps))
    return lax.ppermute(value, axis, [(source, source + steps) for source in range(initial, last)])


def z_shift(value, steps):
    count = lax.axis_size("tp")
    return lax.ppermute(value, "tp", [(i, (i + 2 * steps) % count) for i in range(count)])


def other_core(value):
    count = lax.axis_size("tp")
    return lax.ppermute(value, "tp", [(i, i ^ 1) for i in range(count)])


def contract_last(a, b):
    return lax.dot_general(a, b, (((1,), (1,)), ((), ())), preferred_element_type=f32)


def expert_kernel(sizes, block, with_token, *refs):
    count = len(sizes)
    pieces = refs[:count]
    gate_a, gate_b, up_a, up_b, down_a, down_b = refs[count : count + 6]
    at = count + 6 + with_token
    outs = refs[at : at + count]
    rows, total = refs[at + count :]
    starts = [sum(sizes[:i]) for i in range(count)]
    for start, size, piece in zip(starts, sizes, pieces):
        rows[start : start + size, :] = piece[...]
    x = rows[...]

    def partial(step):
        at = pl.ds(pl.multiple_of(step * block, block), block)
        both = lambda a, b: jnp.concatenate([a[at, :], b[at, :]], axis=0)
        gate_val = contract_last(x, both(gate_a, gate_b))
        up_val = contract_last(x, both(up_a, up_b))
        hidden = (jax.nn.silu(gate_val) * up_val).astype(bf16)
        return jnp.dot(hidden, both(down_a, down_b), preferred_element_type=f32)

    total[...] = jnp.zeros_like(total)

    @pl.loop(0, gate_a.shape[0] // block)
    def _(step):
        total[...] += partial(step)

    for start, size, out in zip(starts, sizes, outs):
        out[...] = total[start : start + size, :].astype(bf16)


def in_vmem(count):
    return [pl.BlockSpec(memory_space=pltpu.VMEM)] * count


def expert(pieces, weights, token=None):
    sizes = tuple(p.shape[0] for p in pieces)
    width = pieces[0].shape[1]
    hidden = weights[0].shape[0]
    tokens = () if token is None else (token,)
    flops = 2 * 3 * sum(sizes) * width * 2 * hidden
    return pl.pallas_call(
        functools.partial(expert_kernel, sizes, hidden // 2, len(tokens)),
        in_specs=in_vmem(len(sizes) + 6) + [pl.BlockSpec(memory_space=pl.ANY)] * len(tokens),
        out_specs=in_vmem(len(sizes)),
        out_shape=[jax.ShapeDtypeStruct((size, width), bf16) for size in sizes],
        scratch_shapes=[
            pltpu.VMEM((sum(sizes), width), bf16),
            pltpu.VMEM((sum(sizes), width), f32),
        ],
        compiler_params=pltpu.CompilerParams(vmem_limit_bytes=VMEM_LIMIT),
        cost_estimate=pl.CostEstimate(flops=flops, bytes_accessed=1 << 20, transcendentals=0),
    )(*pieces, *weights, *tokens)


def gated(value, gate):
    value, gate = value.astype(f32), gate.astype(f32)
    return (value * jax.nn.sigmoid(gate)).astype(bf16)


def position_major(lanes):
    pair = TILE // 4
    last = lanes.shape[1] - TILE
    here = lanes[:, :last]
    ahead = jnp.concatenate([lanes[:, pair:last], lanes[:, last : last + pair]], axis=1)
    return jnp.concatenate([here, ahead], axis=0).T


def tap_sum(laid, start, rows, taps):
    count = taps.shape[0]
    total = jnp.zeros((rows, laid.shape[1]), f32)
    for j in range(count):
        total = total + taps[j : j + 1, :] * laid[start + j : start + j + rows, :]
    return total.astype(bf16)


def twice(taps):
    return jnp.concatenate([taps[...], taps[...]], axis=1)


def conv_main_kernel(line, taps, out, laid):
    blocks, rows, _ = out.shape
    both = twice(taps)
    line = line[...].astype(f32)
    line = jnp.concatenate([line, jnp.zeros((line.shape[0], TILE), f32)], axis=1)
    laid[...] = position_major(line)
    lead = both.shape[0] - 1

    @pl.loop(1, blocks)
    def _(block):
        window = laid[pl.ds(pl.multiple_of(2 * rows * (block - 1) + rows, rows), 2 * rows), :]
        out[block, :, :] = tap_sum(window, rows - lead, rows, both)


def conv_first_kernel(rim, line, taps, _, out, laid):
    rows = out.shape[1]
    both = twice(taps)
    line = line[...].astype(f32)
    line = jnp.concatenate([rim[...].astype(f32), line, jnp.zeros_like(line)], axis=1)
    laid[...] = position_major(line)
    lead = both.shape[0] - 1
    out[0, :, :] = tap_sum(laid, rim.shape[1] - lead, rows, both)


def convolve(line, taps, rim, blocks):
    channels, length = line.shape
    rows = length // blocks // 2
    shape = jax.ShapeDtypeStruct((blocks, rows, 2 * channels), bf16)
    main = pl.pallas_call(
        conv_main_kernel,
        in_specs=in_vmem(2),
        out_specs=in_vmem(1)[0],
        out_shape=shape,
        scratch_shapes=[pltpu.VMEM((length, 2 * channels), f32)],
        compiler_params=pltpu.CompilerParams(vmem_limit_bytes=4 << 20),
        cost_estimate=pl.CostEstimate(flops=5 << 28, bytes_accessed=1 << 20, transcendentals=0),
    )(line, taps)
    return pl.pallas_call(
        conv_first_kernel,
        grid=(1,),
        in_specs=[
            pl.BlockSpec(rim.shape, lambda i: (0, 0)),
            pl.BlockSpec((channels, TILE), lambda i: (0, 0)),
            pl.BlockSpec(taps.shape, lambda i: (0, 0)),
            pl.BlockSpec(memory_space=pl.ANY),
        ],
        out_specs=pl.BlockSpec((1, rows, 2 * channels), lambda i: (0, 0, 0)),
        out_shape=shape,
        scratch_shapes=[pltpu.VMEM((rim.shape[1] + TILE, 2 * channels), f32)],
        input_output_aliases={3: 0},
        compiler_params=pltpu.CompilerParams(vmem_limit_bytes=4 << 20),
        cost_estimate=pl.CostEstimate(flops=1 << 27, bytes_accessed=1 << 16, transcendentals=0),
    )(rim, line, taps, main)


def token_kernel(
    conv,
    gain,
    bias,
    out_weight,
    stream,
    expert_gain,
    routes,
    route_weights,
    send,
    residual,
    mixer_hi,
    mixer_lo,
):
    top, tokens = routes.shape
    slot_count = send.shape[0]
    capacity = slot_count // EXPERTS
    names = lax.broadcasted_iota(jnp.int32, (EXPERTS, tokens), 0)
    hits = [(names == routes[k : k + 1, :]).astype(f32) for k in range(top)]
    earlier = lax.broadcasted_iota(jnp.int32, (tokens, tokens), 0) < lax.broadcasted_iota(
        jnp.int32, (tokens, tokens), 1
    )
    before = jnp.dot(
        sum(hits).astype(bf16), earlier.astype(bf16), preferred_element_type=f32
    )
    places = lax.broadcasted_iota(jnp.int32, (slot_count, tokens), 0)
    chooser = jnp.zeros((slot_count, tokens), f32)
    weighted = jnp.zeros((slot_count, tokens), f32)
    for k in range(top):
        rank = jnp.sum(before * hits[k], axis=0, keepdims=True).astype(jnp.int32)
        taken = places == routes[k : k + 1, :] * capacity + rank
        chooser = chooser + jnp.where(taken, 1.0, 0.0)
        weighted = weighted + jnp.where(taken, route_weights[k : k + 1, :], 0.0)
        before = before + hits[k]
    upper = weighted.astype(bf16)
    mixer_hi[...] = upper
    mixer_lo[...] = (weighted - upper.astype(f32)).astype(bf16)

    parts, _, lanes = conv.shape
    half = lanes // 2
    x = jnp.concatenate(
        [
            jnp.concatenate([conv[p, :, :half] for p in range(parts)], axis=1),
            jnp.concatenate([conv[p, :, half:] for p in range(parts)], axis=1),
        ],
        axis=0,
    ).astype(f32)
    center = jnp.mean(x, axis=1, keepdims=True)
    x = x - center
    spread = jnp.mean(x * x, axis=1, keepdims=True)
    scaled = x * lax.rsqrt(spread + epsilon) * gain[...] + bias[...]
    active = jax.nn.silu(scaled).astype(bf16)
    projected = jnp.dot(active, out_weight[...], preferred_element_type=f32)
    kept = (stream[...].astype(f32) + projected).astype(bf16)
    residual[...] = kept
    kept = kept.astype(f32)
    scale = lax.rsqrt(jnp.mean(kept * kept, axis=1, keepdims=True) + epsilon)
    normed = (kept * scale * expert_gain[...]).astype(bf16)
    send[...] = jnp.dot(chooser.astype(bf16), normed, preferred_element_type=f32).astype(bf16)


def token_block(conv, gain, bias, out_weight, stream, expert_gain, routes, route_weights):
    top, tokens = routes.shape
    return pl.pallas_call(
        token_kernel,
        in_specs=in_vmem(8),
        out_specs=in_vmem(4),
        out_shape=[
            jax.ShapeDtypeStruct((top * tokens, stream.shape[1]), bf16),
            jax.ShapeDtypeStruct(stream.shape, bf16),
            jax.ShapeDtypeStruct((top * tokens, tokens), bf16),
            jax.ShapeDtypeStruct((top * tokens, tokens), bf16),
        ],
        compiler_params=pltpu.CompilerParams(vmem_limit_bytes=12 << 20),
        cost_estimate=pl.CostEstimate(flops=3 << 29, bytes_accessed=5 << 20, transcendentals=0),
    )(
        conv,
        gain[None, :],
        bias[None, :],
        out_weight,
        stream,
        expert_gain[None, :],
        routes,
        route_weights,
    )


def add_kernel(a, b, out):
    out[...] = (a[...].astype(f32) + b[...].astype(f32)).astype(bf16)


def add(a, b):
    return pl.pallas_call(
        add_kernel,
        out_shape=jax.ShapeDtypeStruct(a.shape, bf16),
        compiler_params=pltpu.CompilerParams(vmem_limit_bytes=4 << 20),
        cost_estimate=pl.CostEstimate(
            flops=a.size * 500, bytes_accessed=a.size * 6, transcendentals=0
        ),
    )(a, b)


def split_kernel(both, first, second):
    half = first.shape[0]
    first[...] = both[:half, :]
    second[...] = both[half:, :]


def split(both):
    half = jax.ShapeDtypeStruct((both.shape[0] // 2, both.shape[1]), both.dtype)
    return pl.pallas_call(
        split_kernel,
        in_specs=in_vmem(1),
        out_specs=in_vmem(2),
        out_shape=[half, half],
        compiler_params=pltpu.CompilerParams(vmem_limit_bytes=4 << 20),
    )(both)


def close_kernel(right_a, left_a, own_a, right_b, left_b, own_b, out):
    half = right_a.shape[0]
    out[:half, :] = (
        right_a[...].astype(f32) + left_a[...].astype(f32) + own_a[...].astype(f32)
    ).astype(bf16)
    out[half:, :] = (
        right_b[...].astype(f32) + left_b[...].astype(f32) + own_b[...].astype(f32)
    ).astype(bf16)


def close(*parts):
    half, width = parts[0].shape
    return pl.pallas_call(
        close_kernel,
        out_shape=jax.ShapeDtypeStruct((2 * half, width), bf16),
        compiler_params=pltpu.CompilerParams(vmem_limit_bytes=4 << 20),
    )(*parts)


def per_device(
    conv_value,
    conv_gate,
    conv_taps,
    norm_gain,
    norm_bias,
    out_weight,
    stream,
    routes,
    route_weights,
    expert_gain,
    expert_gate,
    expert_up,
    expert_down,
):
    run_len = conv_value.shape[1]
    line = lax.optimization_barrier(gated(conv_value, conv_gate))
    rim = shifted(line[:, run_len - TILE :], "sp", 1)
    blocks = lax.axis_size("tp")
    conv_out = convolve(line, conv_taps.T, rim, blocks)
    tok_rows = stream.shape[0]
    width = stream.shape[1]
    top_count = routes.shape[1]
    experts = lax.axis_size("sp")
    capacity = top_count * tok_rows // experts
    whole_conv = lax.all_to_all(conv_out, "tp", split_axis=0, concat_axis=0, tiled=True)
    send_rows, residual, mixer_hi, mixer_lo = token_block(
        whole_conv,
        norm_gain,
        norm_bias,
        out_weight,
        stream,
        expert_gain,
        routes.T,
        route_weights.T,
    )
    mine = (expert_gate[0].T, expert_up[0].T, expert_down[0])
    send_rows, gone = lax.optimization_barrier((send_rows, mine))
    weights = [w for pair in zip(mine, map(other_core, gone)) for w in pair]
    send_rows = send_rows.reshape(experts, capacity, width)
    received = lax.all_to_all(send_rows, "sp", split_axis=0, concat_axis=0, tiled=True)
    received, weights = lax.optimization_barrier((received, weights))
    own = received.reshape(-1, width)

    far = lax.axis_size("tp") // 4
    from_left = {0: tuple(split(own))}
    from_right = {0: from_left[0]}
    for k in range(1, far + 1):
        left_a, left_b = from_left[k - 1]
        right_a, right_b = from_right[k - 1]
        left_a = z_shift(left_a, 1)
        right_b = z_shift(right_b, -1)
        left_b = z_shift(left_b, 1) if k < far else None
        right_a = z_shift(right_a, -1) if k < far else None
        from_left[k] = (left_a, left_b)
        from_right[k] = (right_a, right_b)

    part_own = expert(from_left[0], weights)
    part_left, part_right = {}, {}
    token = part_own[0]
    for k in range(2, far):
        parts = expert((*from_left[k], *from_right[k]), weights, token)
        part_left[k], part_right[k] = parts[0:2], parts[2:4]
        token = parts[0]
    right_b = z_shift(part_right[far - 1][1], 1)
    left_a = z_shift(part_left[far - 1][0], -1)
    antipode = expert((from_left[far][0], from_right[far][1]), weights, token)

    right_a = z_shift(antipode[0], 1)
    left_b = z_shift(antipode[1], -1)
    parts = expert((*from_left[1], *from_right[1]), weights, antipode[0])
    part_left[1], part_right[1] = parts[0:2], parts[2:4]
    for k in range(far - 1, 0, -1):
        if k < far - 1:
            right_b = z_shift(add(right_b, part_right[k][1]), 1)
            left_a = z_shift(add(left_a, part_left[k][0]), -1)
        right_a = z_shift(add(right_a, part_right[k][0]), 1)
        left_b = z_shift(add(left_b, part_left[k][1]), -1)
    result = close(right_a, left_a, part_own[0], right_b, left_b, part_own[1])
    result = result.reshape(received.shape)
    returned = lax.all_to_all(result, "sp", split_axis=0, concat_axis=0, tiled=True)
    rows = returned.reshape(experts * capacity, width)

    def mix(weight):
        return lax.dot_general(weight, rows, (((0,), (0,)), ((), ())), preferred_element_type=f32)

    expert_sum = mix(mixer_hi) + mix(mixer_lo)
    return (residual.astype(f32) + expert_sum).astype(bf16)


def solution(mesh):
    return jax.shard_map(
        per_device,
        mesh=mesh,
        in_specs=(
            P("tp", "sp"),
            P("tp", "sp"),
            P("tp", None),
            P(),
            P(),
            P(),
            P(("sp", "tp"), None),
            P(("sp", "tp"), None),
            P(("sp", "tp"), None),
            P(),
            P("sp", None, "tp"),
            P("sp", None, "tp"),
            P("sp", "tp", None),
        ),
        out_specs=P(("sp", "tp"), None),
        check_vma=False,
    )
```

```python
import functools
import jax
import jax.numpy as jnp
from jax import lax
from jax.experimental import pallas as pl
from jax.experimental.pallas import tpu as pltpu
from jax.sharding import PartitionSpec as P


epsilon = 1e-06
f32 = jnp.float32
bf16 = jnp.bfloat16
VMEM_LIMIT = 12 << 20
TILE = 128
EXPERTS = 16


def shifted(value, axis, steps):
    count = lax.axis_size(axis)
    initial, last = (max(0, -steps), min(count, count - steps))
    return lax.ppermute(value, axis, [(source, source + steps) for source in range(initial, last)])


def z_shift(value, steps):
    count = lax.axis_size("tp")
    return lax.ppermute(value, "tp", [(i, (i + 2 * steps) % count) for i in range(count)])


def other_core(value):
    count = lax.axis_size("tp")
    return lax.ppermute(value, "tp", [(i, i ^ 1) for i in range(count)])


def contract_last(a, b):
    return lax.dot_general(a, b, (((1,), (1,)), ((), ())), preferred_element_type=f32)


def expert_kernel(sizes, block, with_token, *refs):
    count = len(sizes)
    pieces = refs[:count]
    gate_a, gate_b, up_a, up_b, down_a, down_b = refs[count : count + 6]
    at = count + 6 + with_token
    outs = refs[at : at + count]
    rows, total = refs[at + count :]
    starts = [sum(sizes[:i]) for i in range(count)]
    for start, size, piece in zip(starts, sizes, pieces):
        rows[start : start + size, :] = piece[...]
    x = rows[...]

    def partial(step):
        at = pl.ds(pl.multiple_of(step * block, block), block)
        both = lambda a, b: jnp.concatenate([a[at, :], b[at, :]], axis=0)
        gate_val = contract_last(x, both(gate_a, gate_b))
        up_val = contract_last(x, both(up_a, up_b))
        hidden = (jax.nn.silu(gate_val) * up_val).astype(bf16)
        return jnp.dot(hidden, both(down_a, down_b), preferred_element_type=f32)

    total[...] = jnp.zeros_like(total)

    @pl.loop(0, gate_a.shape[0] // block)
    def _(step):
        total[...] += partial(step)

    for start, size, out in zip(starts, sizes, outs):
        out[...] = total[start : start + size, :].astype(bf16)


def in_vmem(count):
    return [pl.BlockSpec(memory_space=pltpu.VMEM)] * count


def expert(pieces, weights, token=None):
    sizes = tuple(p.shape[0] for p in pieces)
    width = pieces[0].shape[1]
    hidden = weights[0].shape[0]
    tokens = () if token is None else (token,)
    flops = 2 * 3 * sum(sizes) * width * 2 * hidden
    return pl.pallas_call(
        functools.partial(expert_kernel, sizes, hidden // 2, len(tokens)),
        in_specs=in_vmem(len(sizes) + 6) + [pl.BlockSpec(memory_space=pl.ANY)] * len(tokens),
        out_specs=in_vmem(len(sizes)),
        out_shape=[jax.ShapeDtypeStruct((size, width), bf16) for size in sizes],
        scratch_shapes=[
            pltpu.VMEM((sum(sizes), width), bf16),
            pltpu.VMEM((sum(sizes), width), f32),
        ],
        compiler_params=pltpu.CompilerParams(vmem_limit_bytes=VMEM_LIMIT),
        cost_estimate=pl.CostEstimate(flops=flops, bytes_accessed=1 << 20, transcendentals=0),
    )(*pieces, *weights, *tokens)


def gated(value, gate):
    value, gate = value.astype(f32), gate.astype(f32)
    return (value * jax.nn.sigmoid(gate)).astype(bf16)


def position_major(lanes):
    pair = TILE // 4
    last = lanes.shape[1] - TILE
    here = lanes[:, :last]
    ahead = jnp.concatenate([lanes[:, pair:last], lanes[:, last : last + pair]], axis=1)
    return jnp.concatenate([here, ahead], axis=0).T


def tap_sum(laid, start, rows, taps):
    count = taps.shape[0]
    total = jnp.zeros((rows, laid.shape[1]), f32)
    for j in range(count):
        total = total + taps[j : j + 1, :] * laid[start + j : start + j + rows, :]
    return total.astype(bf16)


def twice(taps):
    return jnp.concatenate([taps[...], taps[...]], axis=1)


def conv_main_kernel(line, taps, out, laid):
    blocks, rows, _ = out.shape
    both = twice(taps)
    line = line[...].astype(f32)
    line = jnp.concatenate([line, jnp.zeros((line.shape[0], TILE), f32)], axis=1)
    laid[...] = position_major(line)
    lead = both.shape[0] - 1

    @pl.loop(1, blocks)
    def _(block):
        window = laid[pl.ds(pl.multiple_of(2 * rows * (block - 1) + rows, rows), 2 * rows), :]
        out[block, :, :] = tap_sum(window, rows - lead, rows, both)


def conv_first_kernel(rim, line, taps, _, out, laid):
    rows = out.shape[1]
    both = twice(taps)
    line = line[...].astype(f32)
    line = jnp.concatenate([rim[...].astype(f32), line, jnp.zeros_like(line)], axis=1)
    laid[...] = position_major(line)
    lead = both.shape[0] - 1
    out[0, :, :] = tap_sum(laid, rim.shape[1] - lead, rows, both)


def convolve(line, taps, rim, blocks):
    channels, length = line.shape
    rows = length // blocks // 2
    shape = jax.ShapeDtypeStruct((blocks, rows, 2 * channels), bf16)
    main = pl.pallas_call(
        conv_main_kernel,
        in_specs=in_vmem(2),
        out_specs=in_vmem(1)[0],
        out_shape=shape,
        scratch_shapes=[pltpu.VMEM((length, 2 * channels), f32)],
        compiler_params=pltpu.CompilerParams(vmem_limit_bytes=4 << 20),
        cost_estimate=pl.CostEstimate(flops=5 << 28, bytes_accessed=1 << 20, transcendentals=0),
    )(line, taps)
    return pl.pallas_call(
        conv_first_kernel,
        grid=(1,),
        in_specs=[
            pl.BlockSpec(rim.shape, lambda i: (0, 0)),
            pl.BlockSpec((channels, TILE), lambda i: (0, 0)),
            pl.BlockSpec(taps.shape, lambda i: (0, 0)),
            pl.BlockSpec(memory_space=pl.ANY),
        ],
        out_specs=pl.BlockSpec((1, rows, 2 * channels), lambda i: (0, 0, 0)),
        out_shape=shape,
        scratch_shapes=[pltpu.VMEM((rim.shape[1] + TILE, 2 * channels), f32)],
        input_output_aliases={3: 0},
        compiler_params=pltpu.CompilerParams(vmem_limit_bytes=4 << 20),
        cost_estimate=pl.CostEstimate(flops=1 << 27, bytes_accessed=1 << 16, transcendentals=0),
    )(rim, line, taps, main)


def token_kernel(
    conv,
    gain,
    bias,
    out_weight,
    stream,
    expert_gain,
    routes,
    route_weights,
    send,
    residual,
    mixer_hi,
    mixer_lo,
):
    top, tokens = routes.shape
    slot_count = send.shape[0]
    capacity = slot_count // EXPERTS
    names = lax.broadcasted_iota(jnp.int32, (EXPERTS, tokens), 0)
    hits = [(names == routes[k : k + 1, :]).astype(f32) for k in range(top)]
    earlier = lax.broadcasted_iota(jnp.int32, (tokens, tokens), 0) < lax.broadcasted_iota(
        jnp.int32, (tokens, tokens), 1
    )
    before = jnp.dot(
        sum(hits).astype(bf16), earlier.astype(bf16), preferred_element_type=f32
    )
    places = lax.broadcasted_iota(jnp.int32, (slot_count, tokens), 0)
    chooser = jnp.zeros((slot_count, tokens), f32)
    weighted = jnp.zeros((slot_count, tokens), f32)
    for k in range(top):
        rank = jnp.sum(before * hits[k], axis=0, keepdims=True).astype(jnp.int32)
        taken = places == routes[k : k + 1, :] * capacity + rank
        chooser = chooser + jnp.where(taken, 1.0, 0.0)
        weighted = weighted + jnp.where(taken, route_weights[k : k + 1, :], 0.0)
        before = before + hits[k]
    upper = weighted.astype(bf16)
    mixer_hi[...] = upper
    mixer_lo[...] = (weighted - upper.astype(f32)).astype(bf16)

    parts, _, lanes = conv.shape
    half = lanes // 2
    x = jnp.concatenate(
        [
            jnp.concatenate([conv[p, :, :half] for p in range(parts)], axis=1),
            jnp.concatenate([conv[p, :, half:] for p in range(parts)], axis=1),
        ],
        axis=0,
    ).astype(f32)
    center = jnp.mean(x, axis=1, keepdims=True)
    x = x - center
    spread = jnp.mean(x * x, axis=1, keepdims=True)
    scaled = x * lax.rsqrt(spread + epsilon) * gain[...] + bias[...]
    active = jax.nn.silu(scaled).astype(bf16)
    projected = jnp.dot(active, out_weight[...], preferred_element_type=f32)
    kept = (stream[...].astype(f32) + projected).astype(bf16)
    residual[...] = kept
    kept = kept.astype(f32)
    scale = lax.rsqrt(jnp.mean(kept * kept, axis=1, keepdims=True) + epsilon)
    normed = (kept * scale * expert_gain[...]).astype(bf16)
    send[...] = jnp.dot(chooser.astype(bf16), normed, preferred_element_type=f32).astype(bf16)


def token_block(conv, gain, bias, out_weight, stream, expert_gain, routes, route_weights):
    top, tokens = routes.shape
    return pl.pallas_call(
        token_kernel,
        in_specs=in_vmem(8),
        out_specs=in_vmem(4),
        out_shape=[
            jax.ShapeDtypeStruct((top * tokens, stream.shape[1]), bf16),
            jax.ShapeDtypeStruct(stream.shape, bf16),
            jax.ShapeDtypeStruct((top * tokens, tokens), bf16),
            jax.ShapeDtypeStruct((top * tokens, tokens), bf16),
        ],
        compiler_params=pltpu.CompilerParams(vmem_limit_bytes=12 << 20),
        cost_estimate=pl.CostEstimate(flops=3 << 29, bytes_accessed=5 << 20, transcendentals=0),
    )(
        conv,
        gain[None, :],
        bias[None, :],
        out_weight,
        stream,
        expert_gain[None, :],
        routes,
        route_weights,
    )


def add_kernel(a, b, out):
    out[...] = (a[...].astype(f32) + b[...].astype(f32)).astype(bf16)


def add(a, b):
    return pl.pallas_call(
        add_kernel,
        out_shape=jax.ShapeDtypeStruct(a.shape, bf16),
        compiler_params=pltpu.CompilerParams(vmem_limit_bytes=4 << 20),
        cost_estimate=pl.CostEstimate(
            flops=a.size * 500, bytes_accessed=a.size * 6, transcendentals=0
        ),
    )(a, b)


def split_kernel(both, first, second):
    half = first.shape[0]
    first[...] = both[:half, :]
    second[...] = both[half:, :]


def split(both):
    half = jax.ShapeDtypeStruct((both.shape[0] // 2, both.shape[1]), both.dtype)
    return pl.pallas_call(
        split_kernel,
        in_specs=in_vmem(1),
        out_specs=in_vmem(2),
        out_shape=[half, half],
        compiler_params=pltpu.CompilerParams(vmem_limit_bytes=4 << 20),
    )(both)


def close_kernel(right_a, left_a, own_a, right_b, left_b, own_b, out):
    half = right_a.shape[0]
    out[:half, :] = (
        right_a[...].astype(f32) + left_a[...].astype(f32) + own_a[...].astype(f32)
    ).astype(bf16)
    out[half:, :] = (
        right_b[...].astype(f32) + left_b[...].astype(f32) + own_b[...].astype(f32)
    ).astype(bf16)


def close(*parts):
    half, width = parts[0].shape
    return pl.pallas_call(
        close_kernel,
        out_shape=jax.ShapeDtypeStruct((2 * half, width), bf16),
        compiler_params=pltpu.CompilerParams(vmem_limit_bytes=4 << 20),
    )(*parts)


def per_device(
    conv_value,
    conv_gate,
    conv_taps,
    norm_gain,
    norm_bias,
    out_weight,
    stream,
    routes,
    route_weights,
    expert_gain,
    expert_gate,
    expert_up,
    expert_down,
):
    run_len = conv_value.shape[1]
    line = lax.optimization_barrier(gated(conv_value, conv_gate))
    rim = shifted(line[:, run_len - TILE :], "sp", 1)
    blocks = lax.axis_size("tp")
    conv_out = convolve(line, conv_taps.T, rim, blocks)
    tok_rows = stream.shape[0]
    width = stream.shape[1]
    top_count = routes.shape[1]
    experts = lax.axis_size("sp")
    capacity = top_count * tok_rows // experts
    whole_conv = lax.all_to_all(conv_out, "tp", split_axis=0, concat_axis=0, tiled=True)
    send_rows, residual, mixer_hi, mixer_lo = token_block(
        whole_conv,
        norm_gain,
        norm_bias,
        out_weight,
        stream,
        expert_gain,
        routes.T,
        route_weights.T,
    )
    send_rows = send_rows.reshape(experts, capacity, width)
    received = lax.all_to_all(send_rows, "sp", split_axis=0, concat_axis=0, tiled=True)
    weights = []
    for mine in (expert_gate[0].T, expert_up[0].T, expert_down[0]):
        weights += [mine, other_core(mine)]
    own = received.reshape(-1, width)

    far = lax.axis_size("tp") // 4
    from_left = {0: tuple(split(own))}
    from_right = {0: from_left[0]}
    for k in range(1, far + 1):
        left_a, left_b = from_left[k - 1]
        right_a, right_b = from_right[k - 1]
        left_a = z_shift(left_a, 1)
        right_b = z_shift(right_b, -1)
        left_b = z_shift(left_b, 1) if k < far else None
        right_a = z_shift(right_a, -1) if k < far else None
        from_left[k] = (left_a, left_b)
        from_right[k] = (right_a, right_b)

    part_left, part_right = {}, {}
    token = None
    for k in range(2, far):
        parts = expert((*from_left[k], *from_right[k]), weights, token)
        part_left[k], part_right[k] = parts[0:2], parts[2:4]
        token = parts[0]
    right_b = z_shift(part_right[far - 1][1], 1)
    left_a = z_shift(part_left[far - 1][0], -1)
    antipode = expert((from_left[far][0], from_right[far][1]), weights, token)

    right_a = z_shift(antipode[0], 1)
    left_b = z_shift(antipode[1], -1)
    parts = expert((*from_left[1], *from_right[1]), weights, antipode[0])
    part_left[1], part_right[1] = parts[0:2], parts[2:4]
    part_own = expert(from_left[0], weights, parts[0])
    for k in range(far - 1, 0, -1):
        if k < far - 1:
            right_b = z_shift(add(right_b, part_right[k][1]), 1)
            left_a = z_shift(add(left_a, part_left[k][0]), -1)
        right_a = z_shift(add(right_a, part_right[k][0]), 1)
        left_b = z_shift(add(left_b, part_left[k][1]), -1)
    result = close(right_a, left_a, part_own[0], right_b, left_b, part_own[1])
    result = result.reshape(received.shape)
    returned = lax.all_to_all(result, "sp", split_axis=0, concat_axis=0, tiled=True)
    rows = returned.reshape(experts * capacity, width)

    def mix(weight):
        return lax.dot_general(weight, rows, (((0,), (0,)), ((), ())), preferred_element_type=f32)

    expert_sum = mix(mixer_hi) + mix(mixer_lo)
    return (residual.astype(f32) + expert_sum).astype(bf16)


def solution(mesh):
    return jax.shard_map(
        per_device,
        mesh=mesh,
        in_specs=(
            P("tp", "sp"),
            P("tp", "sp"),
            P("tp", None),
            P(),
            P(),
            P(),
            P(("sp", "tp"), None),
            P(("sp", "tp"), None),
            P(("sp", "tp"), None),
            P(),
            P("sp", None, "tp"),
            P("sp", None, "tp"),
            P("sp", "tp", None),
        ),
        out_specs=P(("sp", "tp"), None),
        check_vma=False,
    )
```
